32 devices in a mesh: grp: 2 (over x), kv: 4 (over z), tp: 4 (over y, core).
Axes of the slice: x: 2, y: 2, z: 4, core: 2. Of those that a mesh axis runs over, the one named last changes fastest.
Arguments:
- x_rows: bfloat16 [256, 4096], P('grp', 'kv'), parts along dimension 0, may hold values from -32 to 32
- in_gain: bfloat16 [4096], P('kv'), may hold values from 0.099609375 to 1.8984375
- query_weight: bfloat16 [4096, 4096], P('kv', 'tp'), may hold values from -0.09375 to 0.09375
- key_weight: bfloat16 [4096, 4096], P('kv', 'tp'), may hold values from -0.09375 to 0.09375
- value_weight: bfloat16 [4096, 8192], P('kv', 'tp'), may hold values from -0.09375 to 0.09375
- outgate_weight: bfloat16 [4096, 8192], P('kv', 'tp'), may hold values from -0.09375 to 0.09375
- input_gate_weight: bfloat16 [4096, 32], P('kv', 'tp'), may hold values from -0.09375 to 0.09375
- forget_gate_weight: bfloat16 [4096, 32], P('kv', 'tp'), may hold values from -0.09375 to 0.09375
- forget_bias: float32 [32], P('tp'), may hold values from -1 to 3
- state_matrix: float32 [256, 32, 128, 256], P(('grp', 'kv'), 'tp'), parts along dimension 0, may hold values from -3 to 3
- state_norm: float32 [256, 32, 128], P(('grp', 'kv'), 'tp'), parts along dimension 0, may hold values from -6 to 6
- state_max: float32 [256, 32], P(('grp', 'kv'), 'tp'), parts along dimension 0, may hold values from -1 to 1
- head_gain: bfloat16 [8192], P('tp'), may hold values from 0.099609375 to 1.8984375
- out_weight: bfloat16 [8192, 4096], P('tp', 'kv'), may hold values from -0.0625 to 0.0625
- mix_gain: bfloat16 [4096], P('kv'), may hold values from 0.099609375 to 1.8984375
- up_weight: bfloat16 [4096, 16384], P('kv', 'tp'), may hold values from -0.09375 to 0.09375
- down_weight: bfloat16 [16384, 4096], P('tp', 'kv'), may hold values from -0.046875 to 0.046875
Outputs:
- mixed_out: bfloat16 [256, 4096], P('grp', 'kv'), parts along dimension 0
- new_matrix: float32 [256, 32, 128, 256], P(('grp', 'kv'), 'tp'), parts along dimension 0
- new_norm: float32 [256, 32, 128], P(('grp', 'kv'), 'tp'), parts along dimension 0
- new_max: float32 [256, 32], P(('grp', 'kv'), 'tp'), parts along dimension 0
The draws below stay inside these ranges and needn't reach their ends.
There are 2 independent parts, one for each index of `grp`. The reference program is written for one: setup_inputs(seed, part) draws one part's arguments, and reference() takes and returns one part's arrays. A program takes and returns all parts, laid end to end along the dimension named above; an argument that names none is the same for every part. Nothing has to cross between parts.
All inputs are finite; a program needn't handle non-finite values.
Results may differ from the reference program's by a relative error of at most 0.019.
Values may be sent and summed in bfloat16 or wider, within the bound.
A program may use at most 192 MiB of HBM per device.

```python
import jax
import jax.numpy as jnp
from jax import lax

D = 4096
H = 32
DQK = 128
DV = 256
FF = 16384
B = 128


def draw_x_rows(key, part):
    first, second, third = jax.random.split(key, 3)
    position = jnp.arange(D, dtype=jnp.float32) / (D - 1)
    rough = jnp.exp(jax.random.uniform(second, (D,), jnp.float32, -0.35, 0.35))
    row_scale = jnp.exp(jax.random.uniform(third, (B, 1), jnp.float32, jnp.log(0.1), jnp.log(1.0)))
    base = jnp.clip(jax.random.normal(first, (B, D), jnp.float32), -4.0, 4.0)
    rising = jnp.exp(jnp.log(3.0) * position)
    return (base * row_scale * (rising * rough)[None, :]).astype(jnp.bfloat16)


def block_scale(key, extent, cuts, low, high):
    def one(dim, blocks):
        heights = jax.random.uniform(jax.random.fold_in(jax.random.fold_in(key, 6), dim), (blocks,), jnp.float32, low / len(cuts), high / len(cuts))
        return jnp.repeat(jnp.exp(heights), extent[dim] // blocks).reshape((-1,) + (1,) * (len(extent) - dim - 1))

    level = one(*cuts[0])
    for cut in cuts[1:]:
        level = level * one(*cut)
    return level


def centred(key, extent, scale, limit, cuts=(), kind=jnp.bfloat16):
    drawn = scale * jax.random.normal(key, extent, jnp.float32)
    if cuts:
        drawn = drawn * block_scale(key, extent, cuts, -0.22, 0.18)
    return jnp.clip(drawn, -limit, limit).astype(kind)


def setup_inputs(seed: int = 0, part: int = 0) -> dict:
    streams_of = jax.random.split(jax.random.key(seed), 18)
    part_splits = jax.random.split(jax.random.fold_in(streams_of[17], part), 18)
    return {
        "x_rows": draw_x_rows(jax.random.fold_in(jax.random.fold_in(streams_of[17], part), 71), part),
        "in_gain": jnp.clip(1.0 + 0.18 * jax.random.normal(streams_of[1], (D,), jnp.float32), 0.099609375, 1.8984375).astype(jnp.bfloat16),
        "query_weight": centred(streams_of[2], (D, H * DQK), D ** -0.5, 0.09375, ((0, 4), (1, 4))),
        "key_weight": centred(streams_of[3], (D, H * DQK), D ** -0.5, 0.09375, ((0, 4), (1, 4))),
        "value_weight": centred(streams_of[4], (D, H * DV), D ** -0.5, 0.09375, ((0, 4), (1, 4))),
        "outgate_weight": centred(streams_of[5], (D, H * DV), D ** -0.5, 0.09375, ((0, 4), (1, 4))),
        "input_gate_weight": centred(streams_of[6], (D, H), D ** -0.5, 0.09375, ((0, 4), (1, 4))),
        "forget_gate_weight": centred(streams_of[7], (D, H), D ** -0.5, 0.09375, ((0, 4), (1, 4))),
        "forget_bias": jnp.clip(-1.0 + 4.0 * jax.random.uniform(streams_of[8], (H,), jnp.float32) ** block_scale(streams_of[8], (H,), ((0, 4),), -0.2, 0.2), -1.0, 3.0),
        "state_matrix": centred(part_splits[9], (B, H, DQK, DV), 0.5, 3.0, ((0, 4), (1, 4)), jnp.float32),
        "state_norm": centred(part_splits[10], (B, H, DQK), 1.0, 6.0, ((0, 4), (1, 4)), jnp.float32),
        "state_max": jnp.clip(jax.random.uniform(part_splits[11], (B, H), jnp.float32, -1.0, 1.0) * block_scale(part_splits[11], (B, H), ((0, 4), (1, 4)), -0.4, 0.0), -1.0, 1.0),
        "head_gain": jnp.clip(1.0 + 0.18 * jax.random.normal(streams_of[12], (H * DV,), jnp.float32), 0.099609375, 1.8984375).astype(jnp.bfloat16),
        "out_weight": centred(streams_of[13], (H * DV, D), (H * DV) ** -0.5, 0.0625, ((0, 4), (1, 4))),
        "mix_gain": jnp.clip(1.0 + 0.18 * jax.random.normal(streams_of[14], (D,), jnp.float32), 0.099609375, 1.8984375).astype(jnp.bfloat16),
        "up_weight": centred(streams_of[15], (D, FF), D ** -0.5, 0.09375, ((0, 4), (1, 4))),
        "down_weight": centred(streams_of[16], (FF, D), FF ** -0.5, 0.046875, ((0, 4), (1, 4))),
    }


epsilon = 1e-06

def reference(x_rows, in_gain, query_weight, key_weight, value_weight, outgate_weight, input_gate_weight, forget_gate_weight, forget_bias, state_matrix, state_norm, state_max, head_gain, out_weight, mix_gain, up_weight, down_weight):
    xfull = x_rows.astype(jnp.float32)
    squares = lax.optimization_barrier(jnp.sum(xfull * xfull, axis=1))
    scale = lax.rsqrt(squares / D + epsilon)[:, None]
    scaled = (xfull * in_gain.astype(jnp.float32)).astype(jnp.bfloat16)

    def project(weight):
        return jnp.dot(scaled, weight, preferred_element_type=jnp.float32) * scale

    def rounded(weight):
        return lax.optimization_barrier(project(weight).astype(jnp.bfloat16)).astype(jnp.float32)
    query = rounded(query_weight).reshape(B, H, DQK) * DQK ** (-0.5)
    keys = rounded(key_weight).reshape(B, H, DQK)
    values = rounded(value_weight).reshape(B, H, DV)
    outgate = rounded(outgate_weight).reshape(B, H, DV)
    igate = project(input_gate_weight)
    fgate = project(forget_gate_weight)
    log_forget = jax.nn.log_sigmoid(fgate + forget_bias[None, :])
    new_max = jnp.maximum(log_forget + state_max, igate)
    fdecay = jnp.exp(log_forget + state_max - new_max)
    idecay = jnp.exp(igate - new_max)
    new_matrix = fdecay[:, :, None, None] * state_matrix + idecay[:, :, None, None] * (keys[:, :, :, None] * values[:, :, None, :])
    new_norm = fdecay[:, :, None] * state_norm + idecay[:, :, None] * keys
    numer = jnp.einsum('bhd,bhde->bhe', query, new_matrix, precision=lax.Precision.HIGHEST)
    denom = lax.optimization_barrier(jnp.sum(query * new_norm, axis=-1))
    readout = numer / jnp.maximum(jnp.abs(denom), jnp.exp(-new_max))[:, :, None]
    normed = readout * lax.rsqrt(lax.optimization_barrier(jnp.mean(readout * readout, axis=-1, keepdims=True)) + epsilon)
    normed = normed * head_gain.astype(jnp.float32).reshape(H, DV)
    merged = (jax.nn.sigmoid(outgate) * normed).reshape(B, H * DV).astype(jnp.bfloat16)
    branch = jnp.dot(merged, out_weight, preferred_element_type=jnp.float32)
    resid = lax.optimization_barrier((xfull + branch).astype(jnp.bfloat16)).astype(jnp.float32)
    scale_two = lax.rsqrt(lax.optimization_barrier(jnp.sum(resid * resid, axis=1)) / D + epsilon)[:, None]
    scaled_two = (resid * mix_gain.astype(jnp.float32)).astype(jnp.bfloat16)
    act = jnp.dot(scaled_two, up_weight, preferred_element_type=jnp.float32) * scale_two
    hidden = jnp.square(jax.nn.relu(act)).astype(jnp.bfloat16)
    down = jnp.dot(hidden, down_weight, preferred_element_type=jnp.float32)
    mixed_out = (resid + down).astype(jnp.bfloat16)
    return (mixed_out, new_matrix, new_norm, new_max)
```

```python
import functools
import math

import jax
import jax.numpy as jnp
from jax import lax
from jax.experimental import pallas as pl
from jax.experimental.pallas import tpu as pltpu
from jax.sharding import PartitionSpec as P

LANES = 128
EPS = 1e-06
MESH = pl.DeviceIdType.MESH
F32 = jnp.float32
BF16 = jnp.bfloat16


def kernel(
    kvn,
    tpn,
    width,
    model,
    x_ref,
    x3_ref,
    gain_ref,
    q_hbm,
    k_hbm,
    v_hbm,
    o_hbm,
    gate_ref,
    bias_ref,
    state_hbm,
    norm_ref,
    max_ref,
    head_gain_ref,
    out_hbm,
    mix_gain_ref,
    up_hbm,
    down_hbm,
    mixed_ref,
    matrix_hbm,
    new_norm_ref,
    new_max_ref,
    weights,
    down_w,
    state,
    scaled,
    part,
    gate_send,
    gate_recv,
    proj_send,
    proj_recv,
    q_all,
    k_all,
    v_all,
    o_all,
    fd_all,
    id_all,
    em_all,
    merged,
    merged_all,
    branch_send,
    branch_recv,
    resid_all,
    sq_send,
    sq_recv,
    up_send,
    up_recv,
    hidden_all,
    mix_send,
    mix_recv,
    mixed_all,
    w_sem,
    w2_sem,
    down_sem,
    state_sem,
    write_sem,
    gate_ss,
    gate_rs,
    proj_ss,
    proj_rs,
    mg_ss,
    mg_rs,
    br_ss,
    br_rs,
    rd_ss,
    rd_rs,
    sq_ss,
    sq_rs,
    up_ss,
    up_rs,
    hd_ss,
    hd_rs,
    mx_ss,
    mx_rs,
    ma_ss,
    ma_rs,
):
    me = lax.axis_index("kv")
    tme = lax.axis_index("tp")
    total, local = x_ref.shape
    rows, heads, dqk = norm_ref.shape
    dv = head_gain_ref.shape[1]
    trows = total // tpn
    tile = min(256, width)
    hidden_units = up_hbm.shape[1]

    def kv_peer(j):
        return lax.rem(me + j, kvn)

    def tp_peer(j):
        return lax.rem(tme + j, tpn)

    def send(src, dst, ssem, rsem, axis, peer):
        copy = pltpu.make_async_remote_copy(
            src_ref=src,
            dst_ref=dst,
            send_sem=ssem,
            recv_sem=rsem,
            device_id={axis: peer},
            device_id_type=MESH,
        )
        copy.start()
        return copy

    sent = []

    first = []
    for name, ref in enumerate((q_hbm, k_hbm, v_hbm, o_hbm)):
        for offset in range(0, ref.shape[1], width):
            first.append((name, ref, offset))
    loads = []
    for c, (name, ref, offset) in enumerate(first):
        copy = pltpu.make_async_copy(
            ref.at[:, pl.ds(offset, width)], weights.at[c], w_sem.at[c]
        )
        copy.start()
        loads.append(copy)
    second = []
    for a in range(0, out_hbm.shape[0], local):
        for b in range(0, out_hbm.shape[1], width):
            second.append((out_hbm, a, b))
    out_blocks = len(second)
    for b in range(0, hidden_units, width):
        second.append((up_hbm, 0, b))

    barrier = pltpu.get_barrier_semaphore()
    for j in range(1, kvn):
        pl.semaphore_signal(barrier, inc=1, device_id={"kv": kv_peer(j)}, device_id_type=MESH)
    for j in range(1, tpn):
        pl.semaphore_signal(barrier, inc=1, device_id={"tp": tp_peer(j)}, device_id_type=MESH)

    xf = x_ref[...].astype(F32)
    squares = jnp.sum(xf * xf, axis=1, keepdims=True)
    scaled[...] = (xf * gain_ref[...].astype(F32)).astype(BF16)
    gates = jnp.dot(scaled[...], gate_ref[...], preferred_element_type=F32)
    gate_send[:, :, 0 : 2 * LANES] = gates.reshape(kvn, rows, 2 * LANES)
    gate_send[:, :, 2 * LANES :] = jnp.broadcast_to(squares, (total, LANES)).reshape(
        kvn, rows, LANES
    )
    pl.semaphore_wait(barrier, (kvn - 1) + (tpn - 1))
    gate_copies = []
    for j in range(1, kvn):
        gate_copies.append(
            send(gate_send.at[kv_peer(j)], gate_recv.at[j - 1], gate_ss.at[j - 1], gate_rs.at[j - 1], "kv", kv_peer(j))
        )
    sent += gate_copies

    def matmul_chunk(lhs, slot, dest, c):
        def body(i, carry):
            cols = pl.ds(pl.multiple_of(i * tile, tile), tile)
            res = jnp.dot(lhs[...], weights[slot, :, cols], preferred_element_type=F32)
            dest[c, :, :, cols] = res.reshape(kvn, rows, tile).astype(BF16)
            return carry

        lax.fori_loop(0, width // tile, body, 0)

    def state_load(r):
        return pltpu.make_async_copy(state_hbm.at[r], state.at[r], state_sem.at[r])

    def state_store(r):
        return pltpu.make_async_copy(state.at[r], matrix_hbm.at[r], write_sem.at[r])

    proj_copies = []
    loads2 = []
    for c in range(len(first)):
        loads[c].wait()
        matmul_chunk(scaled, c, proj_send, c)
        for j in range(1, kvn):
            proj_copies.append(
                send(
                    proj_send.at[c, kv_peer(j)],
                    proj_recv.at[c, j - 1],
                    proj_ss.at[c, j - 1],
                    proj_rs.at[c, j - 1],
                    "kv",
                    kv_peer(j),
                )
            )
    sent += proj_copies
    for r in range(rows):
        state_load(r).start()
    for c, (ref, a, b) in enumerate(second):
        copy = pltpu.make_async_copy(
            ref.at[pl.ds(a, local), pl.ds(b, width)], weights.at[c], w2_sem.at[c]
        )
        copy.start()
        loads2.append(copy)
    down_load = pltpu.make_async_copy(down_hbm, down_w, down_sem.at[0])
    down_load.start()

    for copy in gate_copies:
        copy.wait_recv()
    gsum = gate_send[me]
    for j in range(1, kvn):
        gsum = gsum + gate_recv[j - 1]
    scale = lax.rsqrt(gsum[:, 2 * LANES : 2 * LANES + 1] / model + EPS)
    igate = gsum[:, 0:heads] * scale
    z = gsum[:, LANES : LANES + heads] * scale + bias_ref[...]
    logf = jnp.minimum(z, 0.0) - jnp.log1p(jnp.exp(-jnp.abs(z)))
    held = logf + max_ref[...]
    new_max = jnp.maximum(held, igate)
    new_max_ref[...] = new_max
    fdec = jnp.exp(held - new_max)
    idec = jnp.exp(igate - new_max)
    floor = jnp.exp(-new_max)
    for h in range(heads):
        for src, dst in ((fdec, fd_all), (idec, id_all), (floor, em_all)):
            dst[:, h, :] = jnp.broadcast_to(src[:, h : h + 1], (rows, LANES))

    targets = ((q_all, dqk), (k_all, dqk), (v_all, dv), (o_all, dv))
    for c, (name, ref, offset) in enumerate(first):
        for j in range(1, kvn):
            proj_copies[c * (kvn - 1) + j - 1].wait_recv()
        dst, extent = targets[name]
        for g in range(0, width, LANES):
            val = proj_send[c, me, :, g : g + LANES].astype(F32)
            for j in range(1, kvn):
                val = val + proj_recv[c, j - 1, :, g : g + LANES].astype(F32)
            val = (val * scale).astype(BF16).astype(F32)
            if name == 0:
                val = val * (dqk ** (-0.5))
            at = offset + g
            col = at % extent
            dst[:, at // extent, col : col + LANES] = val

    pad = jnp.zeros((LANES - 2 * heads, dqk), F32)

    def row_body(r, carry):
        state_load(r).wait()
        q8, k8, v8, o8 = q_all[r], k_all[r], v_all[r], o_all[r]
        fd8, id8, em8 = fd_all[r], id_all[r], em_all[r]
        ik8 = id8 * k8
        turned = jnp.concatenate([ik8, q8, pad], axis=0).T
        numer = []
        for h in range(heads):
            fd = jnp.concatenate([fd8[h : h + 1, :]] * (dv // LANES), axis=1)
            new = fd * state[r, h] + turned[:, h : h + 1] * v8[h : h + 1, :]
            state[r, h] = new
            numer.append(
                jnp.sum(turned[:, heads + h : heads + h + 1] * new, axis=0, keepdims=True)
            )
        state_store(r).start()
        numer = jnp.concatenate(numer, axis=0)
        nn = fd8 * norm_ref[r] + ik8
        new_norm_ref[r] = nn
        denom = jnp.sum(q8 * nn, axis=1, keepdims=True)
        readout = numer / jnp.maximum(jnp.abs(denom), em8[:, 0:1])
        normed = readout * lax.rsqrt(
            jnp.sum(readout * readout, axis=1, keepdims=True) / dv + EPS
        )
        merged[r] = jax.nn.sigmoid(o8) * (normed * head_gain_ref[...])
        return carry

    lax.fori_loop(0, rows, row_body, 0)

    for h in range(heads):
        merged_all[me, :, h * dv : (h + 1) * dv] = merged[:, h, :].astype(BF16)
    mg = []
    for j in range(1, kvn):
        mg.append(
            send(merged_all.at[me], merged_all.at[me], mg_ss.at[j - 1], mg_rs.at[j - 1], "kv", kv_peer(j))
        )
    sent += mg
    for c in range(out_blocks):
        loads2[c].wait()
    for copy in mg:
        copy.wait_recv()
    for b in range(0, local, width):

        def out_body(i, carry, b=b):
            cols = pl.ds(pl.multiple_of(i * tile, tile), tile)
            acc = jnp.zeros((total, tile), F32)
            for c in range(out_blocks):
                _, a, bb = second[c]
                if bb != b:
                    continue
                lhs = merged_all[:, :, a : a + local].reshape(total, local)
                acc = acc + jnp.dot(lhs, weights[c, :, cols], preferred_element_type=F32)
            part[:, pl.ds(pl.multiple_of(b + i * tile, tile), tile)] = acc
            return carry

        lax.fori_loop(0, width // tile, out_body, 0)

    def reduce_tp(buf_send, buf_recv, ssem, rsem):
        for j in range(tpn):
            buf_send[j] = part[j * trows : (j + 1) * trows, :].astype(BF16)
        copies = []
        for j in range(1, tpn):
            copies.append(
                send(buf_send.at[tp_peer(j)], buf_recv.at[j - 1], ssem.at[j - 1], rsem.at[j - 1], "tp", tp_peer(j))
            )
        for copy in copies:
            copy.wait_recv()
        val = buf_send[tme].astype(F32)
        for j in range(1, tpn):
            val = val + buf_recv[j - 1].astype(F32)
        return val, copies

    def gather_tp(buf, ssem, rsem):
        copies = []
        for j in range(1, tpn):
            copies.append(
                send(buf.at[tme], buf.at[tme], ssem.at[j - 1], rsem.at[j - 1], "tp", tp_peer(j))
            )
        for copy in copies:
            copy.wait_recv()
        return copies

    branch, copies = reduce_tp(branch_send, branch_recv, br_ss, br_rs)
    sent += copies
    resid_all[tme] = (x3_ref[tme].astype(F32) + branch).astype(BF16)
    sent += gather_tp(resid_all, rd_ss, rd_rs)

    for j in range(tpn):
        part[j * trows : (j + 1) * trows, :] = resid_all[j].astype(F32)
    rf = part[...]
    sq = jnp.sum(rf * rf, axis=1, keepdims=True)
    scaled[...] = (rf * mix_gain_ref[...].astype(F32)).astype(BF16)
    sq_send[...] = jnp.broadcast_to(sq, (total, LANES)).reshape(kvn, rows, LANES)
    sq_copies = []
    for j in range(1, kvn):
        sq_copies.append(
            send(sq_send.at[kv_peer(j)], sq_recv.at[j - 1], sq_ss.at[j - 1], sq_rs.at[j - 1], "kv", kv_peer(j))
        )
    sent += sq_copies
    chunks = hidden_units // width
    up_copies = []
    for c in range(chunks):
        loads2[out_blocks + c].wait()
        matmul_chunk(scaled, out_blocks + c, up_send, c)
        for j in range(1, kvn):
            up_copies.append(
                send(
                    up_send.at[c, kv_peer(j)],
                    up_recv.at[c, j - 1],
                    up_ss.at[c, j - 1],
                    up_rs.at[c, j - 1],
                    "kv",
                    kv_peer(j),
                )
            )
    sent += up_copies
    for copy in sq_copies:
        copy.wait_recv()
    sq_sum = sq_send[me]
    for j in range(1, kvn):
        sq_sum = sq_sum + sq_recv[j - 1]
    scale_two = lax.rsqrt(sq_sum[:, 0:1] / model + EPS)
    hidden_copies = []
    for c in range(chunks):
        for j in range(1, kvn):
            up_copies[c * (kvn - 1) + j - 1].wait_recv()
        val = up_send[c, me].astype(F32)
        for j in range(1, kvn):
            val = val + up_recv[c, j - 1].astype(F32)
        act = jnp.maximum(val * scale_two, 0.0)
        hidden_all[c, me] = (act * act).astype(BF16)
        for j in range(1, kvn):
            hidden_copies.append(
                send(
                    hidden_all.at[c, me],
                    hidden_all.at[c, me],
                    hd_ss.at[c, j - 1],
                    hd_rs.at[c, j - 1],
                    "kv",
                    kv_peer(j),
                )
            )
    sent += hidden_copies
    down_load.wait()
    for c in range(chunks):
        for j in range(1, kvn):
            hidden_copies[c * (kvn - 1) + j - 1].wait_recv()

        def down_body(i, carry, c=c):
            cols = pl.ds(pl.multiple_of(i * tile, tile), tile)
            lhs = hidden_all[c].reshape(total, width)
            res = jnp.dot(
                lhs, down_w[c * width : (c + 1) * width, cols], preferred_element_type=F32
            )
            if c == 0:
                part[:, cols] = res
            else:
                part[:, cols] += res
            return carry

        lax.fori_loop(0, local // tile, down_body, 0)
    down, copies = reduce_tp(mix_send, mix_recv, mx_ss, mx_rs)
    sent += copies
    mixed_all[tme] = (resid_all[tme].astype(F32) + down).astype(BF16)
    sent += gather_tp(mixed_all, ma_ss, ma_rs)
    mixed_ref[...] = mixed_all[...]

    for copy in sent:
        copy.wait_send()

    def drain(r, carry):
        state_store(r).wait()
        return carry

    lax.fori_loop(0, rows, drain, 0)


def per_device(
    kvn,
    tpn,
    x_rows,
    in_gain,
    query_weight,
    key_weight,
    value_weight,
    outgate_weight,
    input_gate_weight,
    forget_gate_weight,
    forget_bias,
    state_matrix,
    state_norm,
    state_max,
    head_gain,
    out_weight,
    mix_gain,
    up_weight,
    down_weight,
):
    total, local = x_rows.shape
    rows, heads, dqk, dv = state_matrix.shape
    trows = total // tpn
    hidden_units = up_weight.shape[1]
    width = functools.reduce(
        math.gcd,
        [local, heads * dqk, heads * dv, hidden_units],
    )
    n_first = (2 * heads * dqk + 2 * heads * dv) // width
    n_second = (heads * dv // local) * (local // width) + hidden_units // width
    chunks = hidden_units // width
    gap = ((0, 0), (0, LANES - heads))
    gate = jnp.concatenate(
        [jnp.pad(input_gate_weight, gap), jnp.pad(forget_gate_weight, gap)], axis=1
    )
    vmem = pl.BlockSpec(memory_space=pltpu.VMEM)
    hbm = pl.BlockSpec(memory_space=pl.ANY)
    V = pltpu.VMEM
    dma = pltpu.SemaphoreType.DMA
    k1, t1 = max(kvn - 1, 1), max(tpn - 1, 1)
    scratch = [
        V((max(n_first, n_second), local, width), BF16),
        V((hidden_units, local), BF16),
        V((rows, heads, dqk, dv), F32),
        V((total, local), BF16),
        V((total, local), F32),
        V((kvn, rows, 3 * LANES), F32),
        V((k1, rows, 3 * LANES), F32),
        V((n_first, kvn, rows, width), BF16),
        V((n_first, k1, rows, width), BF16),
        V((rows, heads, dqk), F32),
        V((rows, heads, dqk), F32),
        V((rows, heads, dv), F32),
        V((rows, heads, dv), F32),
        V((rows, heads, LANES), F32),
        V((rows, heads, LANES), F32),
        V((rows, heads, LANES), F32),
        V((rows, heads, dv), F32),
        V((kvn, rows, heads * dv), BF16),
        V((tpn, trows, local), BF16),
        V((t1, trows, local), BF16),
        V((tpn, trows, local), BF16),
        V((kvn, rows, LANES), F32),
        V((k1, rows, LANES), F32),
        V((chunks, kvn, rows, width), BF16),
        V((chunks, k1, rows, width), BF16),
        V((chunks, kvn, rows, width), BF16),
        V((tpn, trows, local), BF16),
        V((t1, trows, local), BF16),
        V((tpn, trows, local), BF16),
        dma((n_first,)),
        dma((n_second,)),
        dma((1,)),
        dma((rows,)),
        dma((rows,)),
        dma((k1,)),
        dma((k1,)),
        dma((n_first, k1)),
        dma((n_first, k1)),
        dma((k1,)),
        dma((k1,)),
        dma((t1,)),
        dma((t1,)),
        dma((t1,)),
        dma((t1,)),
        dma((k1,)),
        dma((k1,)),
        dma((chunks, k1)),
        dma((chunks, k1)),
        dma((chunks, k1)),
        dma((chunks, k1)),
        dma((t1,)),
        dma((t1,)),
        dma((t1,)),
        dma((t1,)),
    ]
    model = local * kvn
    mixed, new_matrix, new_norm, new_max = pl.pallas_call(
        functools.partial(kernel, kvn, tpn, width, model),
        out_shape=(
            jax.ShapeDtypeStruct((tpn, trows, local), BF16),
            jax.ShapeDtypeStruct(state_matrix.shape, F32),
            jax.ShapeDtypeStruct(state_norm.shape, F32),
            jax.ShapeDtypeStruct(state_max.shape, F32),
        ),
        in_specs=[vmem, vmem, vmem, hbm, hbm, hbm, hbm, vmem, vmem, hbm, vmem, vmem, vmem, hbm, vmem, hbm, hbm],
        out_specs=(vmem, hbm, vmem, vmem),
        scratch_shapes=scratch,
        compiler_params=pltpu.CompilerParams(
            collective_id=0, has_side_effects=True, vmem_limit_bytes=67043328
        ),
    )(
        x_rows,
        x_rows.reshape(tpn, trows, local),
        in_gain.reshape(1, local),
        query_weight,
        key_weight,
        value_weight,
        outgate_weight,
        gate,
        forget_bias.reshape(1, heads),
        state_matrix,
        state_norm,
        state_max,
        head_gain.astype(F32).reshape(heads, dv),
        out_weight,
        mix_gain.reshape(1, local),
        up_weight,
        down_weight,
    )
    return (mixed.reshape(total, local), new_matrix, new_norm, new_max)


def solution(mesh):
    placed = (
        P("grp", "kv"),
        P("kv"),
        P("kv", "tp"),
        P("kv", "tp"),
        P("kv", "tp"),
        P("kv", "tp"),
        P("kv", "tp"),
        P("kv", "tp"),
        P("tp"),
        P(("grp", "kv"), "tp", None, None),
        P(("grp", "kv"), "tp", None),
        P(("grp", "kv"), "tp"),
        P("tp"),
        P("tp", "kv"),
        P("kv"),
        P("kv", "tp"),
        P("tp", "kv"),
    )
    return jax.shard_map(
        functools.partial(per_device, mesh.shape["kv"], mesh.shape["tp"]),
        mesh=mesh,
        in_specs=placed,
        out_specs=(
            P("grp", "kv"),
            P(("grp", "kv"), "tp", None, None),
            P(("grp", "kv"), "tp", None),
            P(("grp", "kv"), "tp"),
        ),
        check_vma=False,
    )
```
